32 devices in a mesh: ep: 4 (over y, x), tp: 8 (over z, core).
Axes of the slice: x: 2, y: 2, z: 4, core: 2. Of those that a mesh axis runs over, the one named last changes fastest.
Arguments:
- stream: bfloat16 [16384, 1024], P(('ep', 'tp')), may hold values from -6 to 6
- norm_gain: float32 [1024], replicated, may hold values from 0.5 to 1.5
- gate_rows: bfloat16 [4, 1024, 1024], P('ep', 'tp'), may hold values from -0.1875 to 0.1875
- up_rows: bfloat16 [4, 1024, 1024], P('ep', 'tp'), may hold values from -0.1875 to 0.1875
- down_rows: bfloat16 [4, 1024, 1024], P('ep', 'tp'), may hold values from -0.1875 to 0.1875
- chosen: int32 [4, 8192], P('ep'), may hold values from 0 to 16383, as said below
- affinity: float32 [4, 8192], P('ep'), may hold values from 0.2 to 1
Outputs:
- mixed_out: bfloat16 [16384, 1024], P(('ep', 'tp'))
The draws below stay inside these ranges and needn't reach their ends.
Inputs may be any that keep to these rules, and one draw needn't show every extreme that they name: Each row of chosen names 8192 different token numbers in increasing order. Among the 512 consecutive token numbers of any one device, an expert reads at most 512, and for every expert some device holds exactly 512 of its tokens.
All inputs are finite; a program needn't handle non-finite values.
Results may differ from the reference program's by a relative error of at most 0.008.
Values may be sent and summed in bfloat16 or wider, within the bound.
A program may use at most 64 MiB of HBM per device.

```python
import jax
import jax.numpy as jnp
from jax import lax

D = 1024
FF = 1024
TOK_DEV = 512
EXPERTS = 4
TOKENS = 16384
CAPACITY = 8192


def draw_chosen(key, part):
    blocks = TOKENS // TOK_DEV
    average = CAPACITY // blocks

    def one_expert(subkey):
        pair_key, offset_key, score_key = jax.random.split(subkey, 3)
        pairing = jax.random.permutation(pair_key, blocks)
        offsets = jax.random.randint(offset_key, (blocks // 2,), 0, average + 1)
        offsets = offsets.at[0].set(average)
        counts = jnp.zeros((blocks,), jnp.int32)
        counts = counts.at[pairing[0::2]].set(average + offsets)
        counts = counts.at[pairing[1::2]].set(average - offsets)
        scores = jax.random.randint(score_key, (blocks, TOK_DEV), 0, 1 << 20) * TOK_DEV
        scores = scores + jnp.arange(TOK_DEV, dtype=jnp.int32)[None, :]
        ranking = jnp.argsort(jnp.argsort(scores, axis=1), axis=1)
        member = (ranking < counts[:, None]).reshape(-1).astype(jnp.int32)
        return jnp.argsort(1 - member, stable=True)[:CAPACITY].astype(jnp.int32)
    expert_keys = jax.random.split(jax.random.fold_in(key, 11), EXPERTS)
    return jax.vmap(one_expert)(expert_keys)


def block_scale(stream_key, extent, shards, low, top_value):
    def one(axis_at, shards_of):
        steps = jax.random.uniform(jax.random.fold_in(jax.random.fold_in(stream_key, 6), axis_at), (shards_of,), jnp.float32, low / len(shards), top_value / len(shards))
        return jnp.repeat(jnp.exp(steps), extent[axis_at] // shards_of).reshape((-1,) + (1,) * (len(extent) - axis_at - 1))

    factor_of = one(*shards[0])
    for cut in shards[1:]:
        factor_of = factor_of * one(*cut)
    return factor_of


def bell_draw(rng, extent, spread, reach, cuts=(), kind=jnp.bfloat16):
    array = jax.random.normal(rng, extent, jnp.float32) * spread
    if len(cuts) > 0:
        array = block_scale(rng, extent, cuts, -0.22, 0.18) * array
    return jnp.clip(array, min=-reach, max=reach).astype(kind)


def setup_inputs(seed: int = 0) -> dict:
    key_list = jax.random.split(jax.random.key(seed), 8)
    return {
        "stream": bell_draw(key_list[0], (TOKENS, D), 1.0, 6.0, ((0, 32),)),
        "norm_gain": jnp.clip(1.0 + 0.1 * jax.random.normal(key_list[1], (D,), jnp.float32), 0.5, 1.5),
        "gate_rows": bell_draw(key_list[2], (EXPERTS, FF, D), D ** -0.5, 0.1875, ((0, 4), (1, 8))),
        "up_rows": bell_draw(key_list[3], (EXPERTS, FF, D), D ** -0.5, 0.1875, ((0, 4), (1, 8))),
        "down_rows": bell_draw(key_list[4], (EXPERTS, FF, D), FF ** -0.5, 0.1875, ((0, 4), (1, 8))),
        "chosen": draw_chosen(jax.random.fold_in(key_list[7], 71), 0),
        "affinity": jnp.clip(0.2 + 0.8 * jax.random.uniform(key_list[6], (EXPERTS, CAPACITY), jnp.float32) ** block_scale(key_list[6], (EXPERTS, CAPACITY), ((0, 4),), -0.2, 0.2), 0.2, 1.0),
    }


epsilon = 1e-06

def reference(stream, norm_gain, gate_rows, up_rows, down_rows, chosen, affinity):
    values = stream.astype(jnp.float32)
    inverse = lax.rsqrt(lax.optimization_barrier(jnp.mean(values * values, axis=-1, keepdims=True)) + epsilon)
    normed = (values * inverse * norm_gain).astype(jnp.bfloat16)

    def one_expert(running, pieces):
        gate_mat, up_mat, down_mat, picked, weights = pieces
        picked_rows = jnp.take(normed, picked, axis=0)
        gate_sum = jnp.dot(picked_rows, gate_mat.T, preferred_element_type=jnp.float32)
        up_sum = jnp.dot(picked_rows, up_mat.T, preferred_element_type=jnp.float32)
        hidden = (jax.nn.silu(gate_sum) * up_sum).astype(jnp.bfloat16)
        result = jnp.dot(hidden, down_mat, preferred_element_type=jnp.float32).astype(jnp.bfloat16)
        result = lax.optimization_barrier(result)
        weighted = result.astype(jnp.float32) * weights[:, None]
        return (running.at[picked].add(weighted), None)
    initial = jnp.zeros(stream.shape, jnp.float32)
    mixed_out, _ = lax.scan(one_expert, initial, (gate_rows, up_rows, down_rows, chosen, affinity))
    return mixed_out.astype(jnp.bfloat16)
```

```python
import functools

import jax
import jax.numpy as jnp
from jax import lax
from jax.experimental import pallas as pl
from jax.experimental.pallas import tpu as pltpu
from jax.sharding import PartitionSpec as P

epsilon = 1e-06


def over_all(piece, axis, dim, step, start):
    def gathered(part):
        return lax.all_gather(part, axis, axis=dim, tiled=True)

    return step(start, jax.tree.map(gathered, piece), jnp.int32(0))


def shortened(array):
    def short(part):
        return part.astype(jnp.bfloat16) if part.dtype == jnp.float32 else part

    return jax.tree.map(short, array)


def normalize(stream, norm_gain):
    values = stream.astype(jnp.float32)
    inverse = lax.rsqrt(jnp.mean(values * values, axis=-1, keepdims=True) + epsilon)
    return (values * inverse * norm_gain).astype(jnp.bfloat16)


def cut_slices(padded, starts, length):
    return jax.vmap(lambda offset: lax.dynamic_slice_in_dim(padded, offset, length))(starts)


def own_slice(listed, padded, boundary, length):
    offset = jnp.searchsorted(listed, boundary).astype(jnp.int32)
    return lax.dynamic_slice_in_dim(padded, offset, length)


def add_slice(inputs, running, pieces):
    gate_piece, up_piece, down_piece = pieces
    gate_sum = jnp.einsum("erd,efd->erf", inputs, gate_piece, preferred_element_type=jnp.float32)
    up_sum = jnp.einsum("erd,efd->erf", inputs, up_piece, preferred_element_type=jnp.float32)
    hidden = (jax.nn.silu(gate_sum) * up_sum).astype(jnp.bfloat16)
    return running + jnp.einsum(
        "erf,efd->erd", hidden, down_piece, preferred_element_type=jnp.float32
    )


def routed(stream, norm_gain, gate_rows, up_rows, down_rows, chosen, affinity):
    ep_count = lax.axis_size("ep")
    tp_count = lax.axis_size("tp")
    row_count, feature_count = stream.shape
    local_experts = chosen.shape[0]
    slot_count = 4 * row_count // (local_experts * ep_count)
    tp_index = lax.axis_index("tp")
    first_token = (lax.axis_index("ep") * tp_count + tp_index) * row_count
    weight_sets = (gate_rows, up_rows, down_rows)
    normed = normalize(stream, norm_gain)
    column_bounds = (jnp.arange(ep_count, dtype=jnp.int32) * tp_count + tp_index) * row_count
    column_starts = jax.vmap(
        lambda listed: jnp.searchsorted(listed, column_bounds).astype(jnp.int32)
    )(chosen)
    padded_weights = jnp.concatenate(
        [affinity, jnp.zeros((local_experts, slot_count), jnp.float32)], axis=1
    )
    slot_weights = jax.vmap(lambda padded, starts: cut_slices(padded, starts, slot_count))(
        padded_weights, column_starts
    )
    slot_weights = jnp.transpose(slot_weights, (1, 0, 2))
    all_lists = lax.all_gather(chosen, "ep", axis=0, tiled=True)
    padded_all = jnp.concatenate(
        [all_lists, jnp.full((all_lists.shape[0], slot_count), -1, jnp.int32)], axis=1
    )
    own_picks = jax.vmap(lambda listed, padded: own_slice(listed, padded, first_token, slot_count))(
        all_lists, padded_all
    )
    own_picks = own_picks.reshape(ep_count, local_experts, slot_count)
    local_rows = own_picks - first_token
    usable = (local_rows >= 0) & (local_rows < row_count)
    safe_rows = jnp.where(usable, local_rows, 0)
    outgoing = jnp.take(normed, safe_rows.reshape(-1), axis=0)
    outgoing = outgoing.reshape(ep_count, local_experts, slot_count, feature_count)
    outgoing = jnp.where(usable[..., None], outgoing, jnp.zeros((), jnp.bfloat16))
    arrived = lax.all_to_all(outgoing, "ep", split_axis=0, concat_axis=0, tiled=True)
    inputs = jnp.transpose(arrived, (1, 0, 2, 3)).reshape(
        local_experts, ep_count * slot_count, feature_count
    )
    initial = jnp.zeros((local_experts, ep_count * slot_count, feature_count), jnp.float32)
    produced = over_all(
        (weight_sets[0], weight_sets[1], weight_sets[2]),
        "tp",
        1,
        lambda running, pieces, anchor: add_slice(inputs, running, pieces),
        initial,
    )
    produced = produced.astype(jnp.bfloat16).reshape(
        local_experts, ep_count, slot_count, feature_count
    )
    produced = jnp.transpose(produced, (1, 0, 2, 3))
    produced = lax.optimization_barrier(produced)
    weighted = produced.astype(jnp.float32) * slot_weights[..., None]
    returned = lax.all_to_all(
        shortened(weighted), "ep", split_axis=0, concat_axis=0, tiled=True
    ).astype(weighted.dtype)
    segment_ids = jnp.where(usable, local_rows, row_count).reshape(-1)
    summed = jax.ops.segment_sum(
        returned.reshape(-1, feature_count), segment_ids, num_segments=row_count + 1
    )
    return summed[:row_count].astype(jnp.bfloat16)


MESH = pl.DeviceIdType.MESH
LANES = 128


def dense_kernel(
    chips,
    stream_ref, gain_ref, gate_ref, up_ref, down_ref, chosen_ref, weight_ref,
    out_ref,
    arrived, normed, full, scale, hidden, far, near_x, near_y, held_x, held_y, own,
    part_a, part_b, back_x, back_y,
    local_sem, give_sem, pass_sem, take_sem,
    token_send, token_pass, token_take, sum_send, sum_take,
):
    ep = lax.axis_index("ep")
    tp = lax.axis_index("tp")
    rows, width = stream_ref.shape
    half = rows // 2
    units = gate_ref.shape[0]
    chip = tp // 2
    core = lax.rem(tp, 2)
    to_x = (jnp.bitwise_xor(ep, 1), tp)
    to_y = (jnp.bitwise_xor(ep, 2), tp)
    sibling = (ep, chip * 2 + 1 - core)
    others = [(ep, lax.rem(chip + k, chips) * 2 + core) for k in range(1, chips)]
    front = pl.ds(0, half)
    rear = pl.ds(half, half)
    mats = (gate_ref, up_ref, down_ref)

    barrier = pltpu.get_barrier_semaphore()
    peers = [to_x, to_y, sibling] + others
    for peer in peers:
        pl.semaphore_signal(barrier, inc=1, device_id=peer, device_id_type=MESH)
    pl.semaphore_wait(barrier, len(peers))

    def remote(source, target, sent, landed, peer):
        return pltpu.make_async_remote_copy(
            src_ref=source, dst_ref=target, send_sem=sent, recv_sem=landed,
            device_id=peer, device_id_type=MESH,
        )

    sends = []

    def launch(*spec):
        copy = remote(*spec)
        copy.start()
        sends.append(copy)

    def landed(target, sem, peer):
        remote(target, target, sem, sem, peer).wait_recv()

    def token(peer, slot, part, index):
        launch(stream_ref.at[part], arrived.at[slot - 1, part], token_send.at[index],
               token_take.at[slot, 0 if part is front else 1], peer)

    def slot_rows(source):
        return pl.ds(pl.multiple_of(source * units, units), units)

    token(to_x, 1, front, 0)
    token(to_y, 2, rear, 1)
    for m in range(3):
        for k in range(1, chips):
            launch(mats[m], full.at[m, slot_rows(tp)], give_sem.at[m, k],
                   take_sem.at[m, tp], others[k - 1])
    token(to_x, 1, rear, 2)
    token(to_y, 2, front, 3)
    for m in range(3):
        launch(mats[m], full.at[m, slot_rows(tp)], give_sem.at[m, 0],
               take_sem.at[m, tp], sibling)
    kept = []
    for m in range(3):
        copy = pltpu.make_async_copy(mats[m], full.at[m, slot_rows(tp)], local_sem.at[m])
        copy.start()
        kept.append(copy)

    def normalize_block(load, slot):
        def step(i, carry):
            at = pl.ds(pl.multiple_of(i * 64, 64), 64)
            values = load(at).astype(jnp.float32)
            inverse = lax.rsqrt(jnp.mean(values * values, axis=-1, keepdims=True) + epsilon)
            normed[slot, at, :] = (values * inverse * gain_ref[...]).astype(jnp.bfloat16)
            return carry

        lax.fori_loop(0, rows // 64, step, 0)

    normalize_block(lambda at: stream_ref[at, :], 0)

    tp_count = 2 * chips
    window = 8 * ((rows // LANES + 1 + 7) // 8)
    list_rows = chosen_ref.shape[0]
    for slot in range(4):
        first = (jnp.bitwise_xor(ep, slot) * tp_count + tp) * rows
        before = (chosen_ref[:, LANES - 1:LANES] < first).astype(jnp.int32)
        start = jnp.minimum(jnp.sum(before), list_rows - window)
        names = chosen_ref[pl.ds(start, window), :]
        values = weight_ref[pl.ds(start, window), :]
        tokens = first + lax.broadcasted_iota(jnp.int32, (rows, LANES), 0)
        total = jnp.zeros((rows, LANES), jnp.float32)
        for r in range(window):
            total += jnp.where(names[r:r + 1, :] == tokens, values[r:r + 1, :], 0.0)
        scale[slot] = jnp.sum(total, axis=1, keepdims=True)

    landed(arrived.at[0, front], token_take.at[1, 0], to_x)
    launch(arrived.at[0, front], arrived.at[2, front], token_pass.at[0],
           token_take.at[3, 0], to_y)
    landed(arrived.at[1, rear], token_take.at[2, 1], to_y)
    launch(arrived.at[1, rear], arrived.at[2, rear], token_pass.at[1],
           token_take.at[3, 1], to_x)

    def hand_on(m, k):
        source = lax.rem(chip + chips - k, chips) * 2 + core
        place = full.at[m, slot_rows(source)]
        landed(place, take_sem.at[m, source], others[k - 1])
        launch(place, place, pass_sem.at[m, k], take_sem.at[m, source], sibling)

    for m in range(3):
        for k in range(1, chips):
            hand_on(m, k)

    landed(arrived.at[0, rear], token_take.at[1, 1], to_x)
    normalize_block(lambda at: arrived[0, at, :], 1)
    landed(arrived.at[1, front], token_take.at[2, 0], to_y)
    normalize_block(lambda at: arrived[1, at, :], 2)
    landed(arrived.at[2, front], token_take.at[3, 0], to_y)
    landed(arrived.at[2, rear], token_take.at[3, 1], to_x)
    normalize_block(lambda at: arrived[2, at, :], 3)

    for copy in kept:
        copy.wait()
    for m in range(3):
        landed(full.at[m, slot_rows(sibling[1])], take_sem.at[m, sibling[1]], sibling)
        for k in range(1, chips):
            source = lax.rem(chip + chips - k, chips) * 2 + 1 - core
            landed(full.at[m, slot_rows(source)], take_sem.at[m, source], sibling)

    tile = min(256, width)

    def expert(slot, keep):
        def rise(i, carry):
            at = pl.ds(pl.multiple_of(i * tile, tile), tile)
            inputs = normed[slot]
            dims = (((1,), (1,)), ((), ()))
            gate = lax.dot_general(inputs, full[0, at, :], dims,
                                   preferred_element_type=jnp.float32)
            up = lax.dot_general(inputs, full[1, at, :], dims,
                                 preferred_element_type=jnp.float32)
            hidden[:, at] = (gate / (1.0 + jnp.exp(-gate)) * up).astype(jnp.bfloat16)
            return carry

        lax.fori_loop(0, full.shape[1] // tile, rise, 0)

        def fall(i, carry):
            at = pl.ds(pl.multiple_of(i * tile, tile), tile)
            result = jnp.dot(hidden[...], full[2, :, at], preferred_element_type=jnp.float32)
            keep(at, result.astype(jnp.bfloat16).astype(jnp.float32) * scale[slot])
            return carry

        lax.fori_loop(0, width // tile, fall, 0)

    def keep_far(at, value):
        far[:, at] = value.astype(jnp.bfloat16)

    def keep_x(at, value):
        near_x[0:half, at] = value[:half].astype(jnp.bfloat16)
        held_x[:, at] = value[half:]

    def keep_y(at, value):
        near_y[half:rows, at] = value[half:].astype(jnp.bfloat16)
        held_y[:, at] = value[:half]

    def keep_own(at, value):
        own[:, at] = value

    expert(3, keep_far)
    launch(far.at[front], part_a, sum_send.at[0], sum_take.at[0], to_x)
    launch(far.at[rear], part_b, sum_send.at[1], sum_take.at[1], to_y)
    expert(1, keep_x)
    launch(near_x.at[front], back_x.at[front], sum_send.at[2], sum_take.at[2], to_x)
    expert(2, keep_y)
    launch(near_y.at[rear], back_y.at[rear], sum_send.at[3], sum_take.at[3], to_y)
    expert(0, keep_own)
    landed(part_a, sum_take.at[0], to_x)
    near_y[0:half, :] = (held_y[...] + part_a[...].astype(jnp.float32)).astype(jnp.bfloat16)
    launch(near_y.at[front], back_y.at[front], sum_send.at[4], sum_take.at[4], to_y)
    landed(part_b, sum_take.at[1], to_y)
    near_x[half:rows, :] = (held_x[...] + part_b[...].astype(jnp.float32)).astype(jnp.bfloat16)
    launch(near_x.at[rear], back_x.at[rear], sum_send.at[5], sum_take.at[5], to_x)
    landed(back_x.at[front], sum_take.at[2], to_x)
    landed(back_y.at[rear], sum_take.at[3], to_y)
    landed(back_y.at[front], sum_take.at[4], to_y)
    out_ref[0:half, :] = (
        own[0:half, :] + back_x[0:half, :].astype(jnp.float32)
        + back_y[0:half, :].astype(jnp.float32)
    ).astype(jnp.bfloat16)
    landed(back_x.at[rear], sum_take.at[5], to_x)
    out_ref[half:rows, :] = (
        own[half:rows, :] + back_x[half:rows, :].astype(jnp.float32)
        + back_y[half:rows, :].astype(jnp.float32)
    ).astype(jnp.bfloat16)
    for copy in sends:
        copy.wait_send()


def dense(stream, norm_gain, gate_rows, up_rows, down_rows, chosen, affinity):
    tp_count = lax.axis_size("tp")
    rows, width = stream.shape
    half = rows // 2
    units = gate_rows.shape[1]
    hidden_count = units * tp_count
    chips = tp_count // 2
    vmem = pl.BlockSpec(memory_space=pltpu.VMEM)
    low, wide = jnp.bfloat16, jnp.float32
    dma = pltpu.SemaphoreType.DMA
    return pl.pallas_call(
        functools.partial(dense_kernel, chips),
        out_shape=jax.ShapeDtypeStruct((rows, width), low),
        in_specs=[vmem] * 7,
        out_specs=vmem,
        scratch_shapes=[
            pltpu.VMEM((3, rows, width), low),
            pltpu.VMEM((4, rows, width), low),
            pltpu.VMEM((3, hidden_count, width), low),
            pltpu.VMEM((4, rows, 1), wide),
            pltpu.VMEM((rows, hidden_count), low),
            pltpu.VMEM((rows, width), low),
            pltpu.VMEM((rows, width), low),
            pltpu.VMEM((rows, width), low),
            pltpu.VMEM((half, width), wide),
            pltpu.VMEM((half, width), wide),
            pltpu.VMEM((rows, width), wide),
            pltpu.VMEM((half, width), low),
            pltpu.VMEM((half, width), low),
            pltpu.VMEM((rows, width), low),
            pltpu.VMEM((rows, width), low),
            dma((3,)), dma((3, chips)), dma((3, chips)), dma((3, tp_count)),
            dma((4,)), dma((2,)), dma((4, 2)), dma((6,)), dma((6,)),
        ],
        compiler_params=pltpu.CompilerParams(
            collective_id=0, has_side_effects=True, vmem_limit_bytes=60 * 1024 * 1024
        ),
    )(
        stream,
        norm_gain.reshape(1, width),
        gate_rows[0],
        up_rows[0],
        down_rows[0],
        chosen.reshape(-1, LANES),
        affinity.reshape(-1, LANES),
    )


def per_device(stream, norm_gain, gate_rows, up_rows, down_rows, chosen, affinity):
    ep_count = lax.axis_size("ep")
    tp_count = lax.axis_size("tp")
    row_count = stream.shape[0]
    local_experts = chosen.shape[0]
    slot_count = 4 * row_count // (local_experts * ep_count)
    if ep_count == 4 and local_experts == 1 and slot_count >= row_count and tp_count % 2 == 0:
        return dense(stream, norm_gain, gate_rows, up_rows, down_rows, chosen, affinity)
    return routed(stream, norm_gain, gate_rows, up_rows, down_rows, chosen, affinity)


def solution(mesh):
    return jax.shard_map(
        per_device,
        mesh=mesh,
        in_specs=(
            P(("ep", "tp"), None),
            P(),
            P("ep", "tp", None),
            P("ep", "tp", None),
            P("ep", "tp", None),
            P("ep", None),
            P("ep", None),
        ),
        out_specs=P(("ep", "tp"), None),
        check_vma=False,
    )
```

```python
import functools

import jax
import jax.numpy as jnp
from jax import lax
from jax.experimental import pallas as pl
from jax.experimental.pallas import tpu as pltpu
from jax.sharding import PartitionSpec as P

epsilon = 1e-06


def over_all(piece, axis, dim, step, start):
    def gathered(part):
        return lax.all_gather(part, axis, axis=dim, tiled=True)

    return step(start, jax.tree.map(gathered, piece), jnp.int32(0))


def shortened(array):
    def short(part):
        return part.astype(jnp.bfloat16) if part.dtype == jnp.float32 else part

    return jax.tree.map(short, array)


def normalize(stream, norm_gain):
    values = stream.astype(jnp.float32)
    inverse = lax.rsqrt(jnp.mean(values * values, axis=-1, keepdims=True) + epsilon)
    return (values * inverse * norm_gain).astype(jnp.bfloat16)


def cut_slices(padded, starts, length):
    return jax.vmap(lambda offset: lax.dynamic_slice_in_dim(padded, offset, length))(starts)


def own_slice(listed, padded, boundary, length):
    offset = jnp.searchsorted(listed, boundary).astype(jnp.int32)
    return lax.dynamic_slice_in_dim(padded, offset, length)


def add_slice(inputs, running, pieces):
    gate_piece, up_piece, down_piece = pieces
    gate_sum = jnp.einsum("erd,efd->erf", inputs, gate_piece, preferred_element_type=jnp.float32)
    up_sum = jnp.einsum("erd,efd->erf", inputs, up_piece, preferred_element_type=jnp.float32)
    hidden = (jax.nn.silu(gate_sum) * up_sum).astype(jnp.bfloat16)
    return running + jnp.einsum(
        "erf,efd->erd", hidden, down_piece, preferred_element_type=jnp.float32
    )


def routed(stream, norm_gain, gate_rows, up_rows, down_rows, chosen, affinity):
    ep_count = lax.axis_size("ep")
    tp_count = lax.axis_size("tp")
    row_count, feature_count = stream.shape
    local_experts = chosen.shape[0]
    slot_count = 4 * row_count // (local_experts * ep_count)
    tp_index = lax.axis_index("tp")
    first_token = (lax.axis_index("ep") * tp_count + tp_index) * row_count
    weight_sets = (gate_rows, up_rows, down_rows)
    normed = normalize(stream, norm_gain)
    column_bounds = (jnp.arange(ep_count, dtype=jnp.int32) * tp_count + tp_index) * row_count
    column_starts = jax.vmap(
        lambda listed: jnp.searchsorted(listed, column_bounds).astype(jnp.int32)
    )(chosen)
    padded_weights = jnp.concatenate(
        [affinity, jnp.zeros((local_experts, slot_count), jnp.float32)], axis=1
    )
    slot_weights = jax.vmap(lambda padded, starts: cut_slices(padded, starts, slot_count))(
        padded_weights, column_starts
    )
    slot_weights = jnp.transpose(slot_weights, (1, 0, 2))
    all_lists = lax.all_gather(chosen, "ep", axis=0, tiled=True)
    padded_all = jnp.concatenate(
        [all_lists, jnp.full((all_lists.shape[0], slot_count), -1, jnp.int32)], axis=1
    )
    own_picks = jax.vmap(lambda listed, padded: own_slice(listed, padded, first_token, slot_count))(
        all_lists, padded_all
    )
    own_picks = own_picks.reshape(ep_count, local_experts, slot_count)
    local_rows = own_picks - first_token
    usable = (local_rows >= 0) & (local_rows < row_count)
    safe_rows = jnp.where(usable, local_rows, 0)
    outgoing = jnp.take(normed, safe_rows.reshape(-1), axis=0)
    outgoing = outgoing.reshape(ep_count, local_experts, slot_count, feature_count)
    outgoing = jnp.where(usable[..., None], outgoing, jnp.zeros((), jnp.bfloat16))
    arrived = lax.all_to_all(outgoing, "ep", split_axis=0, concat_axis=0, tiled=True)
    inputs = jnp.transpose(arrived, (1, 0, 2, 3)).reshape(
        local_experts, ep_count * slot_count, feature_count
    )
    initial = jnp.zeros((local_experts, ep_count * slot_count, feature_count), jnp.float32)
    produced = over_all(
        (weight_sets[0], weight_sets[1], weight_sets[2]),
        "tp",
        1,
        lambda running, pieces, anchor: add_slice(inputs, running, pieces),
        initial,
    )
    produced = produced.astype(jnp.bfloat16).reshape(
        local_experts, ep_count, slot_count, feature_count
    )
    produced = jnp.transpose(produced, (1, 0, 2, 3))
    produced = lax.optimization_barrier(produced)
    weighted = produced.astype(jnp.float32) * slot_weights[..., None]
    returned = lax.all_to_all(
        shortened(weighted), "ep", split_axis=0, concat_axis=0, tiled=True
    ).astype(weighted.dtype)
    segment_ids = jnp.where(usable, local_rows, row_count).reshape(-1)
    summed = jax.ops.segment_sum(
        returned.reshape(-1, feature_count), segment_ids, num_segments=row_count + 1
    )
    return summed[:row_count].astype(jnp.bfloat16)


MESH = pl.DeviceIdType.MESH
LANES = 128


def dense_kernel(
    chips,
    stream_ref, gain_ref, gate_ref, up_ref, down_ref, chosen_ref, weight_ref,
    out_ref,
    arrived, normed, full, scale, hidden, far, near_x, near_y, held_x, held_y, own,
    part_a, part_b, back_x, back_y,
    local_sem, give_sem, pass_sem, side_sem, take_sem,
    token_send, token_pass, token_take, sum_send, sum_take,
):
    ep = lax.axis_index("ep")
    tp = lax.axis_index("tp")
    rows, width = stream_ref.shape
    half = rows // 2
    units = gate_ref.shape[0]
    chip = tp // 2
    core = lax.rem(tp, 2)
    to_x = (jnp.bitwise_xor(ep, 1), tp)
    to_y = (jnp.bitwise_xor(ep, 2), tp)
    sibling = (ep, chip * 2 + 1 - core)
    has_left = chip > 0
    has_right = chip < chips - 1
    left = (ep, tp - 2)
    right = (ep, tp + 2)
    front = pl.ds(0, half)
    rear = pl.ds(half, half)
    mats = (gate_ref, up_ref, down_ref)

    barrier = pltpu.get_barrier_semaphore()
    peers = ((True, to_x), (True, to_y), (True, sibling), (has_left, left), (has_right, right))
    for there, peer in peers:
        @pl.when(there)
        def _():
            pl.semaphore_signal(barrier, inc=1, device_id=peer, device_id_type=MESH)
    pl.semaphore_wait(
        barrier, 3 + has_left.astype(jnp.int32) + has_right.astype(jnp.int32)
    )

    def remote(source, target, sent, landed, peer):
        return pltpu.make_async_remote_copy(
            src_ref=source, dst_ref=target, send_sem=sent, recv_sem=landed,
            device_id=peer, device_id_type=MESH,
        )

    sends = []

    def launch(*spec, there=True):
        @pl.when(there)
        def _():
            remote(*spec).start()
        sends.append((there, spec))

    def landed(target, sem, peer):
        remote(target, target, sem, sem, peer).wait_recv()

    def token(peer, slot, part, index):
        launch(stream_ref.at[part], arrived.at[slot - 1, part], token_send.at[index],
               token_take.at[slot, 0 if part is front else 1], peer)

    def slot_rows(source):
        return pl.ds(pl.multiple_of(source * units, units), units)

    token(to_x, 1, front, 0)
    token(to_y, 2, rear, 1)
    def give(m):
        place = full.at[m, slot_rows(tp)]
        landing = take_sem.at[m, tp]
        launch(mats[m], place, give_sem.at[m, 0], landing, left, there=has_left)
        launch(mats[m], place, give_sem.at[m, 1], landing, right, there=has_right)
        launch(mats[m], place, give_sem.at[m, 2], landing, sibling)

    give(0)
    give(1)
    token(to_x, 1, rear, 2)
    token(to_y, 2, front, 3)
    kept = []
    for m in range(3):
        copy = pltpu.make_async_copy(mats[m], full.at[m, slot_rows(tp)], local_sem.at[m])
        copy.start()
        kept.append(copy)

    def normalize_block(load, slot):
        def step(i, carry):
            at = pl.ds(pl.multiple_of(i * 64, 64), 64)
            values = load(at).astype(jnp.float32)
            inverse = lax.rsqrt(jnp.mean(values * values, axis=-1, keepdims=True) + epsilon)
            normed[slot, at, :] = (values * inverse * gain_ref[...]).astype(jnp.bfloat16)
            return carry

        lax.fori_loop(0, rows // 64, step, 0)

    normalize_block(lambda at: stream_ref[at, :], 0)

    tp_count = 2 * chips
    window = 8 * ((rows // LANES + 1 + 7) // 8)
    list_rows = chosen_ref.shape[0]
    for slot in range(4):
        first = (jnp.bitwise_xor(ep, slot) * tp_count + tp) * rows
        before = (chosen_ref[:, LANES - 1:LANES] < first).astype(jnp.int32)
        start = jnp.minimum(jnp.sum(before), list_rows - window)
        names = chosen_ref[pl.ds(start, window), :]
        values = weight_ref[pl.ds(start, window), :]
        tokens = first + lax.broadcasted_iota(jnp.int32, (rows, LANES), 0)
        total = jnp.zeros((rows, LANES), jnp.float32)
        for r in range(window):
            total += jnp.where(names[r:r + 1, :] == tokens, values[r:r + 1, :], 0.0)
        scale[slot] = jnp.sum(total, axis=1, keepdims=True)

    def hand_on(m, k):
        for side, there, origin, source_chip, onward, more in (
            (0, chip >= k, left, chip - k, right, has_right),
            (1, chip + k < chips, right, chip + k, left, has_left),
        ):
            source = source_chip * 2 + core
            place = full.at[m, slot_rows(source)]
            landing = take_sem.at[m, source]

            @pl.when(there)
            def _():
                landed(place, landing, origin)

            launch(place, place, pass_sem.at[m, side, k], landing, onward,
                   there=jnp.logical_and(there, more))
            launch(place, place, side_sem.at[m, side, k], landing, sibling, there=there)

    def from_sibling(m):
        for j in range(chips):
            source = j * 2 + 1 - core
            landed(full.at[m, slot_rows(source)], take_sem.at[m, source], sibling)

    for k in range(1, chips):
        if k == 2 or chips == 2:
            give(2)
        hand_on(0, k)
        hand_on(1, k)
        if k == 1:
            landed(arrived.at[0, front], token_take.at[1, 0], to_x)
            launch(arrived.at[0, front], arrived.at[2, front], token_pass.at[0],
                   token_take.at[3, 0], to_y)
            landed(arrived.at[1, rear], token_take.at[2, 1], to_y)
            launch(arrived.at[1, rear], arrived.at[2, rear], token_pass.at[1],
                   token_take.at[3, 1], to_x)

    tile = min(256, width)

    def rise_block(slot):
        def rise(i, carry):
            at = pl.ds(pl.multiple_of(i * tile, tile), tile)
            inputs = normed[slot]
            dims = (((1,), (1,)), ((), ()))
            gate = lax.dot_general(inputs, full[0, at, :], dims,
                                   preferred_element_type=jnp.float32)
            up = lax.dot_general(inputs, full[1, at, :], dims,
                                 preferred_element_type=jnp.float32)
            hidden[slot, :, at] = (gate / (1.0 + jnp.exp(-gate)) * up).astype(jnp.bfloat16)
            return carry

        lax.fori_loop(0, full.shape[1] // tile, rise, 0)

    def fall_block(slot, keep):
        def fall(i, carry):
            at = pl.ds(pl.multiple_of(i * tile, tile), tile)
            result = jnp.dot(hidden[slot], full[2, :, at], preferred_element_type=jnp.float32)
            keep(at, result.astype(jnp.bfloat16).astype(jnp.float32) * scale[slot])
            return carry

        lax.fori_loop(0, width // tile, fall, 0)

    for copy in kept:
        copy.wait()
    from_sibling(0)
    from_sibling(1)
    later = list(range(1, chips))
    for slot in range(4):
        if slot == 1:
            landed(arrived.at[0, rear], token_take.at[1, 1], to_x)
            normalize_block(lambda at: arrived[0, at, :], 1)
        elif slot == 2:
            landed(arrived.at[1, front], token_take.at[2, 0], to_y)
            normalize_block(lambda at: arrived[1, at, :], 2)
        elif slot == 3:
            landed(arrived.at[2, front], token_take.at[3, 0], to_y)
            landed(arrived.at[2, rear], token_take.at[3, 1], to_x)
            normalize_block(lambda at: arrived[2, at, :], 3)
        rise_block(slot)
        for k in later[:1] if slot < 3 else later:
            hand_on(2, k)
        later = later[1:] if slot < 3 else []
    from_sibling(2)

    def keep_far(at, value):
        far[:, at] = value.astype(jnp.bfloat16)

    def keep_x(at, value):
        near_x[0:half, at] = value[:half].astype(jnp.bfloat16)
        held_x[:, at] = value[half:]

    def keep_y(at, value):
        near_y[half:rows, at] = value[half:].astype(jnp.bfloat16)
        held_y[:, at] = value[:half]

    def keep_own(at, value):
        own[:, at] = value

    fall_block(3, keep_far)
    launch(far.at[front], part_a, sum_send.at[0], sum_take.at[0], to_x)
    launch(far.at[rear], part_b, sum_send.at[1], sum_take.at[1], to_y)
    fall_block(1, keep_x)
    launch(near_x.at[front], back_x.at[front], sum_send.at[2], sum_take.at[2], to_x)
    fall_block(2, keep_y)
    launch(near_y.at[rear], back_y.at[rear], sum_send.at[3], sum_take.at[3], to_y)
    fall_block(0, keep_own)
    landed(part_a, sum_take.at[0], to_x)
    near_y[0:half, :] = (held_y[...] + part_a[...].astype(jnp.float32)).astype(jnp.bfloat16)
    launch(near_y.at[front], back_y.at[front], sum_send.at[4], sum_take.at[4], to_y)
    landed(part_b, sum_take.at[1], to_y)
    near_x[half:rows, :] = (held_x[...] + part_b[...].astype(jnp.float32)).astype(jnp.bfloat16)
    launch(near_x.at[rear], back_x.at[rear], sum_send.at[5], sum_take.at[5], to_x)
    landed(back_x.at[front], sum_take.at[2], to_x)
    landed(back_y.at[rear], sum_take.at[3], to_y)
    landed(back_y.at[front], sum_take.at[4], to_y)
    out_ref[0:half, :] = (
        own[0:half, :] + back_x[0:half, :].astype(jnp.float32)
        + back_y[0:half, :].astype(jnp.float32)
    ).astype(jnp.bfloat16)
    landed(back_x.at[rear], sum_take.at[5], to_x)
    out_ref[half:rows, :] = (
        own[half:rows, :] + back_x[half:rows, :].astype(jnp.float32)
        + back_y[half:rows, :].astype(jnp.float32)
    ).astype(jnp.bfloat16)
    for there, spec in sends:
        @pl.when(there)
        def _():
            remote(*spec).wait_send()


def dense(stream, norm_gain, gate_rows, up_rows, down_rows, chosen, affinity):
    tp_count = lax.axis_size("tp")
    rows, width = stream.shape
    half = rows // 2
    units = gate_rows.shape[1]
    hidden_count = units * tp_count
    chips = tp_count // 2
    vmem = pl.BlockSpec(memory_space=pltpu.VMEM)
    low, wide = jnp.bfloat16, jnp.float32
    dma = pltpu.SemaphoreType.DMA
    return pl.pallas_call(
        functools.partial(dense_kernel, chips),
        out_shape=jax.ShapeDtypeStruct((rows, width), low),
        in_specs=[vmem] * 7,
        out_specs=vmem,
        scratch_shapes=[
            pltpu.VMEM((3, rows, width), low),
            pltpu.VMEM((4, rows, width), low),
            pltpu.VMEM((3, hidden_count, width), low),
            pltpu.VMEM((4, rows, 1), wide),
            pltpu.VMEM((4, rows, hidden_count), low),
            pltpu.VMEM((rows, width), low),
            pltpu.VMEM((rows, width), low),
            pltpu.VMEM((rows, width), low),
            pltpu.VMEM((half, width), wide),
            pltpu.VMEM((half, width), wide),
            pltpu.VMEM((rows, width), wide),
            pltpu.VMEM((half, width), low),
            pltpu.VMEM((half, width), low),
            pltpu.VMEM((rows, width), low),
            pltpu.VMEM((rows, width), low),
            dma((3,)), dma((3, 3)), dma((3, 2, chips)), dma((3, 2, chips)), dma((3, tp_count)),
            dma((4,)), dma((2,)), dma((4, 2)), dma((6,)), dma((6,)),
        ],
        compiler_params=pltpu.CompilerParams(
            collective_id=0, has_side_effects=True, vmem_limit_bytes=60 * 1024 * 1024
        ),
    )(
        stream,
        norm_gain.reshape(1, width),
        gate_rows[0],
        up_rows[0],
        down_rows[0],
        chosen.reshape(-1, LANES),
        affinity.reshape(-1, LANES),
    )


def per_device(stream, norm_gain, gate_rows, up_rows, down_rows, chosen, affinity):
    ep_count = lax.axis_size("ep")
    tp_count = lax.axis_size("tp")
    row_count = stream.shape[0]
    local_experts = chosen.shape[0]
    slot_count = 4 * row_count // (local_experts * ep_count)
    if ep_count == 4 and local_experts == 1 and slot_count >= row_count and tp_count % 2 == 0:
        return dense(stream, norm_gain, gate_rows, up_rows, down_rows, chosen, affinity)
    return routed(stream, norm_gain, gate_rows, up_rows, down_rows, chosen, affinity)


def solution(mesh):
    return jax.shard_map(
        per_device,
        mesh=mesh,
        in_specs=(
            P(("ep", "tp"), None),
            P(),
            P("ep", "tp", None),
            P("ep", "tp", None),
            P("ep", "tp", None),
            P("ep", None),
            P("ep", None),
        ),
        out_specs=P(("ep", "tp"), None),
        check_vma=False,
    )
```
